32 devices in a mesh: sp: 8 (over z, y), tp: 4 (over x, core).
Axes of the slice: x: 2, y: 2, z: 4, core: 2. Of those that a mesh axis runs over, the one named last changes fastest.
Arguments:
- resid: bfloat16 [3072, 2048], P('sp', 'tp'), may hold values from -6 to 6
- mixer_in: bfloat16 [3072, 2048], P('sp', 'tp'), may hold values from -6 to 6
- log_step: float32 [3072, 128], P('sp', 'tp'), may hold values from -5.2 to -0.79
- decay_real: float32 [128, 64], P('tp'), may hold values from 0.00016276042 to 0.8
- frequency: float32 [128, 64], P('tp'), may hold values from 0.5 to 6
- input_matrix: float32 [2, 128, 64, 16], P(None, 'tp'), may hold values from -1 to 1
- output_matrix: float32 [2, 128, 16, 64], P(None, 'tp'), may hold values from -0.5 to 0.5
- skip_gain: float32 [2048], P('tp'), may hold values from -4 to 4
- value_weight: bfloat16 [2048, 2048], P(None, 'tp'), may hold values from -0.125 to 0.125
- gate_weight: bfloat16 [2048, 2048], P(None, 'tp'), may hold values from -0.125 to 0.125
- norm_gain: float32 [2048], replicated, may hold values from 0.1 to 1.9
- up_weight: bfloat16 [2048, 8192], P('sp', 'tp'), may hold values from -0.125 to 0.125
- down_weight: bfloat16 [2048, 8192], P('sp', 'tp'), may hold values from -0.0625 to 0.0625
Outputs:
- result: bfloat16 [3072, 2048], P('sp', 'tp')
The draws below stay inside these ranges and needn't reach their ends.
All inputs are finite; a program needn't handle non-finite values.
Results may differ from the reference program's by a relative error of at most 0.014.
Values may be sent and summed in bfloat16 or wider, within the bound.
A program may use at most 128 MiB of HBM per device.

```python
import math
import jax
import jax.numpy as jnp
from jax import lax

D = 2048
FF = 8192
GC = 16
N = 64
TOK_DEV = 384
G = 128
TOKENS = 3072
FF_BLOCK = 2048
N_TP = 4


def draw_log_step(key, part):
    subkeys = jax.random.split(key, 3)
    device_count = TOKENS // TOK_DEV
    device_shift = jax.random.uniform(subkeys[0], (device_count, 1, 1), jnp.float32, -0.7, 0.7)
    group_shift = jax.random.uniform(subkeys[1], (1, 1, G), jnp.float32, -0.5, 0.5)
    jitter = jnp.clip(0.35 * jax.random.normal(subkeys[2], (device_count, TOK_DEV, G), jnp.float32), -1.0, 1.0)
    return (math.log(0.05) + device_shift + group_shift + jitter).reshape(TOKENS, G)


def draw_decay_real(key, part):
    subkeys = jax.random.split(key, 3)
    slow_share = 0.5
    chooser = jax.random.uniform(subkeys[0], (G, N), jnp.float32)
    slow_rate = jnp.exp(jax.random.uniform(subkeys[1], (G, N), jnp.float32, math.log(0.5), math.log(8.0))) / TOKENS
    fast_rate = jnp.exp(jax.random.uniform(subkeys[2], (G, N), jnp.float32, math.log(0.3), math.log(0.8)))
    return jnp.where(chooser < slow_share, slow_rate, fast_rate)


def shard_levels(rng, extent, cuts, smallest, high):
    factor_of = 1.0
    for dim, shards_of in cuts:
        steps = jax.random.uniform(jax.random.fold_in(jax.random.fold_in(rng, 6), dim), (shards_of,), jnp.float32, smallest / len(cuts), high / len(cuts))
        factor_of = factor_of * jnp.repeat(jnp.exp(steps), extent[dim] // shards_of).reshape((-1,) + (1,) * (len(extent) - 1 - dim))
    return factor_of


def normal_values(rng, shape, scale, most, cuts=(), held_as=jnp.bfloat16):
    factor_of = shard_levels(rng, shape, cuts, -0.22, 0.18) if cuts else 1.0
    drawn = jax.random.normal(rng, shape, jnp.float32) * scale * factor_of
    return jnp.minimum(jnp.maximum(drawn, -most), most).astype(held_as)


def setup_inputs(seed: int = 0) -> dict:
    streams_of = jax.random.split(jax.random.key(seed), 14)
    resid = normal_values(streams_of[0], (TOKENS, D), 1.0, 6.0, ((0, 8), (1, 4)))
    mixer_in = normal_values(streams_of[1], (TOKENS, D), 1.0, 6.0, ((0, 8), (1, 4)))
    log_step = draw_log_step(jax.random.fold_in(streams_of[13], 71), 0)
    decay_real = draw_decay_real(jax.random.fold_in(streams_of[13], 71), 0)
    frequency = jnp.clip(0.5 + 5.5 * jax.random.uniform(streams_of[4], (G, N), jnp.float32) ** shard_levels(streams_of[4], (G, N), ((0, 4),), -0.2, 0.2), 0.5, 6.0)
    input_matrix = normal_values(streams_of[5], (2, G, N, GC), (2 * GC) ** -0.5, 1.0, ((1, 4),), jnp.float32)
    output_matrix = normal_values(streams_of[6], (2, G, GC, N), (2 * N) ** -0.5, 0.5, ((1, 4),), jnp.float32)
    skip_gain = normal_values(streams_of[7], (D,), 1.0, 4.0, ((0, 4),), jnp.float32)
    value_weight = normal_values(streams_of[8], (D, D), D ** -0.5, 0.125, ((1, 4),))
    gate_weight = normal_values(streams_of[9], (D, D), D ** -0.5, 0.125, ((1, 4),))
    norm_gain = jnp.clip(1.0 + 0.18 * jax.random.normal(streams_of[10], (D,), jnp.float32), 0.1, 1.9)
    up_weight = normal_values(streams_of[11], (D, FF), D ** -0.5, 0.125, ((0, 8), (1, 4)))
    down_weight = normal_values(streams_of[12], (D, FF), FF ** -0.5, 0.0625, ((0, 8), (1, 4)))
    return dict(resid=resid, mixer_in=mixer_in, log_step=log_step, decay_real=decay_real, frequency=frequency, input_matrix=input_matrix, output_matrix=output_matrix, skip_gain=skip_gain, value_weight=value_weight, gate_weight=gate_weight, norm_gain=norm_gain, up_weight=up_weight, down_weight=down_weight)


rms_eps = 1e-06
highest = lax.Precision.HIGHEST

def chain_link(earlier, later):
    return (earlier[0] * later[0] - earlier[1] * later[1], earlier[0] * later[1] + earlier[1] * later[0], later[0] * earlier[2] - later[1] * earlier[3] + later[2], later[0] * earlier[3] + later[1] * earlier[2] + later[3])

def discretize(log_step, decay_real, frequency):
    states = decay_real.shape[1]
    step_size = jnp.repeat(jnp.exp(log_step), states, axis=1)
    decay_rate = decay_real.reshape(-1)
    angular = frequency.reshape(-1)
    shrink = -decay_rate * step_size
    rotation = angular * step_size
    factor = jnp.exp(shrink)
    decay_re = factor * jnp.cos(rotation)
    decay_im = factor * jnp.sin(rotation)
    half_sine = jnp.sin(0.5 * rotation)
    minus_re = jnp.expm1(shrink) * jnp.cos(rotation) - 2.0 * half_sine * half_sine
    minus_im = decay_im
    modulus = decay_rate * decay_rate + angular * angular
    drive_re = (minus_im * angular - minus_re * decay_rate) / modulus
    drive_im = (-minus_im * decay_rate - minus_re * angular) / modulus
    return (decay_re, decay_im, drive_re, drive_im)

def local_states(mixer_in, log_step, decay_real, frequency, input_matrix):
    tokens = mixer_in.shape[0]
    groups, states = decay_real.shape
    signal = mixer_in.astype(jnp.float32).reshape(tokens, groups, -1)
    proj_re = jnp.einsum('tgk,gnk->tgn', signal, input_matrix[0], precision=highest).reshape(tokens, groups * states)
    proj_im = jnp.einsum('tgk,gnk->tgn', signal, input_matrix[1], precision=highest).reshape(tokens, groups * states)
    decay_re, decay_im, drive_re, drive_im = discretize(log_step, decay_real, frequency)
    feed_re = drive_re * proj_re - drive_im * proj_im
    feed_im = drive_re * proj_im + drive_im * proj_re
    return lax.associative_scan(chain_link, (decay_re, decay_im, feed_re, feed_im), axis=0)

def read_out(state_re, state_im, output_matrix):
    tokens = state_re.shape[0]
    groups = output_matrix.shape[1]
    grid_re = state_re.reshape(tokens, groups, -1)
    grid_im = state_im.reshape(tokens, groups, -1)
    output = jnp.einsum('tgn,gkn->tgk', grid_re, output_matrix[0], precision=highest)
    output = output - jnp.einsum('tgn,gkn->tgk', grid_im, output_matrix[1], precision=highest)
    return output.reshape(tokens, -1)

def reference(resid, mixer_in, log_step, decay_real, frequency, input_matrix, output_matrix, skip_gain, value_weight, gate_weight, norm_gain, up_weight, down_weight):
    group_span = G // N_TP

    def one_block(block_index):
        first_group = block_index * group_span
        columns = lax.dynamic_slice_in_dim(mixer_in, first_group * GC, group_span * GC, 1)
        steps_part = lax.dynamic_slice_in_dim(log_step, first_group, group_span, 1)
        decay_part = lax.dynamic_slice_in_dim(decay_real, first_group, group_span, 0)
        angular = lax.dynamic_slice_in_dim(frequency, first_group, group_span, 0)
        matrix_in = lax.dynamic_slice_in_dim(input_matrix, first_group, group_span, 1)
        matrix_out = lax.dynamic_slice_in_dim(output_matrix, first_group, group_span, 1)
        _, _, state_re, state_im = local_states(columns, steps_part, decay_part, angular, matrix_in)
        return read_out(state_re, state_im, matrix_out)
    outputs = lax.map(one_block, jnp.arange(N_TP, dtype=jnp.int32))
    mechanism = jnp.transpose(outputs, (1, 0, 2)).reshape(TOKENS, D) + skip_gain * mixer_in.astype(jnp.float32)
    mixed_out = jax.nn.gelu(mechanism).astype(jnp.bfloat16)
    value_pre = jnp.dot(mixed_out, value_weight, preferred_element_type=jnp.float32)
    gate_pre = jnp.dot(mixed_out, gate_weight, preferred_element_type=jnp.float32)
    updated = (resid.astype(jnp.float32) + value_pre * jax.nn.sigmoid(gate_pre)).astype(jnp.bfloat16)
    updated_wide = lax.optimization_barrier(updated).astype(jnp.float32)
    inv_rms = lax.rsqrt(lax.optimization_barrier(jnp.mean(updated_wide * updated_wide, axis=1, keepdims=True)) + rms_eps)
    normed = (updated_wide * inv_rms * norm_gain).astype(jnp.bfloat16)
    raised = jnp.dot(normed, up_weight, preferred_element_type=jnp.float32)
    active = jax.nn.relu(raised)
    hidden = (active * active).astype(jnp.bfloat16)

    def add_block(running, block_index):
        start_unit = block_index * FF_BLOCK
        hidden_part = lax.dynamic_slice_in_dim(hidden, start_unit, FF_BLOCK, 1)
        weight_part = lax.dynamic_slice_in_dim(down_weight, start_unit, FF_BLOCK, 1)
        product = lax.dot_general(hidden_part, weight_part, (((1,), (1,)), ((), ())), preferred_element_type=jnp.float32).astype(jnp.bfloat16)
        product = lax.optimization_barrier(product)
        return (running + product.astype(jnp.float32), None)
    down_sum, _ = lax.scan(add_block, jnp.zeros((TOKENS, D), jnp.float32), jnp.arange(N_TP, dtype=jnp.int32))
    return (updated_wide + down_sum).astype(jnp.bfloat16)
```

```python
import functools

import jax
import jax.numpy as jnp
from jax import lax
from jax.experimental import pallas as pl
from jax.experimental.pallas import tpu as pltpu
from jax.sharding import PartitionSpec as P

rms_eps = 1e-06
segments = 8
MESH = pl.DeviceIdType.MESH
f32, bf16 = jnp.float32, jnp.bfloat16


def sine_cosine(x):
    y = x * x
    s = 1.0 + y * (-1 / 6 + y * (1 / 120 + y * (-1 / 5040 + y * (1 / 362880 + y * (-1 / 39916800)))))
    c = 1.0 + y * (
        -0.5
        + y * (1 / 24 + y * (-1 / 720 + y * (1 / 40320 + y * (-1 / 3628800 + y * (1 / 479001600)))))
    )
    return x * s, c


def expm1_small(y):
    return y * (
        1.0
        + y * (1 / 2 + y * (1 / 6 + y * (1 / 24 + y * (1 / 120 + y * (1 / 720 + y * (1 / 5040))))))
    )


def kernel(
    n,
    ntp,
    resid_ref,
    mixer_ref,
    step_ref,
    rates_ref,
    w_in_ref,
    w_out_ref,
    skip_ref,
    value_ref,
    gate_ref,
    gain_ref,
    up_ref,
    down_ref,
    perm_ref,
    unperm_ref,
    out_ref,
    whole,
    dre,
    dim,
    fre,
    fim,
    step_wide,
    proj,
    ends,
    carries,
    entry,
    mixer_perm,
    mixed_perm,
    chan,
    upd,
    normed,
    hidden,
    parts,
    landed,
    ring_send,
    ring_recv,
    own_sem,
    carry_send,
    carry_recv,
    chan_send,
    chan_recv,
    upd_send,
    upd_recv,
    part_send,
    part_recv,
):
    sp = lax.axis_index("sp")
    tp = lax.axis_index("tp")
    tokens, width = mixer_ref.shape
    block = up_ref.shape[0]
    pieces = ring_send.shape[3]
    piece = block // (2 * pieces)
    chunks = w_in_ref.shape[0]
    lanes = w_in_ref.shape[2] // 2
    kin = w_in_ref.shape[1]
    length = tokens // segments

    odd = sp % 2
    pos = (1 - odd) * (sp // 2) + odd * (n - 1 - sp // 2)

    def at_pos(p):
        p = (p + 2 * n) % n
        high = p // (n // 2)
        return (1 - high) * 2 * p + high * (2 * (n - 1 - p) + 1)

    ahead, behind = at_pos(pos + 1), at_pos(pos - 1)

    barrier = pltpu.get_barrier_semaphore()
    for i in range(1, n):
        pl.semaphore_signal(barrier, inc=1, device_id=((sp + i) % n, tp), device_id_type=MESH)
    for i in range(1, ntp):
        pl.semaphore_signal(barrier, inc=1, device_id=(sp, (tp + i) % ntp), device_id_type=MESH)
    pl.semaphore_wait(barrier, n - 1 + ntp - 1)

    def rows_of(owner, way, part):
        return pl.ds(pl.multiple_of(owner * block + (way * pieces + part) * piece, piece), piece)

    def ring_copy(which, way, k, part, sending):
        source = (up_ref, down_ref)[which]
        sign = -1 if way == 0 else 1
        to = ahead if way == 0 else behind
        shift = k if sending else k + 1
        owner = at_pos(pos + sign * shift)
        slot = whole.at[which, rows_of(owner, way, part)]
        if k == 0 and sending:
            src = source.at[pl.ds((way * pieces + part) * piece, piece)]
        else:
            src = slot
        return pltpu.make_async_remote_copy(
            src_ref=src,
            dst_ref=slot,
            send_sem=ring_send.at[which, way, k, part],
            recv_sem=ring_recv.at[which, way, k, part],
            device_id=(to, tp),
            device_id_type=MESH,
        )

    def service(index):
        which, k = index // (n - 1), index % (n - 1)
        for part in range(pieces):
            for way in range(2):
                if k > 0:
                    ring_copy(which, way, k - 1, part, False).wait_recv()
                ring_copy(which, way, k, part, True).start()

    def finish(which):
        for part in range(pieces):
            for way in range(2):
                ring_copy(which, way, n - 2, part, False).wait_recv()

    queue = list(range(2 * (n - 1)))

    def serve(count=1):
        for _ in range(count):
            if queue:
                service(queue.pop(0))

    own = []
    for which, source in enumerate((up_ref, down_ref)):
        start = pl.multiple_of(sp * block, block)
        c = pltpu.make_async_copy(source, whole.at[which, pl.ds(start, block)], own_sem.at[which])
        c.start()
        own.append(c)
    serve()

    mixer_perm[...] = jnp.dot(
        perm_ref[...], mixer_ref[...], preferred_element_type=f32
    ).astype(bf16)
    step_size = jnp.exp(step_ref[...])
    groups = step_size.shape[1]
    for c in range(chunks):
        cols = pl.ds(c * lanes, lanes)
        span = lanes * chunks // groups
        spread = (
            lax.broadcasted_iota(jnp.int32, (groups, lanes), 0) * span
            - lax.broadcasted_iota(jnp.int32, (groups, lanes), 1)
            - c * lanes
        )
        spread = jnp.where((spread <= 0) & (spread > -span), 1.0, 0.0).astype(f32)
        step_wide[...] = jnp.dot(
            step_size, spread, precision=lax.Precision.HIGHEST, preferred_element_type=f32
        )
        proj[...] = jnp.dot(
            mixer_perm[:, c * kin : (c + 1) * kin], w_in_ref[c], preferred_element_type=f32
        )
        shape = (segments, lanes)
        rate = jnp.broadcast_to(rates_ref[0:1, cols], shape)
        half_angle = jnp.broadcast_to(rates_ref[1:2, cols], shape) * 0.5
        rate_n = jnp.broadcast_to(rates_ref[2:3, cols], shape)
        angle_n = jnp.broadcast_to(rates_ref[3:4, cols], shape)

        def one(j, state):
            pr, pi, sr, si = state
            rows = pl.ds(pl.multiple_of(j * segments, segments), segments)
            step = step_wide[rows, :]
            s, co = sine_cosine(half_angle * step)
            em = expm1_small(-rate * step)
            factor = 1.0 + em
            twice = 2.0 * s * s
            cos_r = 1.0 - twice
            dr = factor * cos_r
            di = factor * (2.0 * s * co)
            mr = em * cos_r - twice
            vr = di * angle_n - mr * rate_n
            vi = -di * rate_n - mr * angle_n
            a = proj[rows, 0:lanes]
            b = proj[rows, lanes : 2 * lanes]
            fr = vr * a - vi * b
            fi = vr * b + vi * a
            dre[rows, cols] = dr
            dim[rows, cols] = di
            fre[rows, cols] = fr
            fim[rows, cols] = fi
            return (
                dr * pr - di * pi,
                dr * pi + di * pr,
                dr * sr - di * si + fr,
                dr * si + di * sr + fi,
            )

        zero = jnp.zeros(shape, f32)
        last = lax.fori_loop(0, length, one, (zero + 1.0, zero, zero, zero), unroll=2)
        for i in range(4):
            ends[i, :, cols] = last[i]
        serve()

    def link(earlier, later):
        return (
            later[0] * earlier[0] - later[1] * earlier[1] + later[2],
            later[0] * earlier[1] + later[1] * earlier[0] + later[3],
        )

    pr, pi, sr, si = (ends[i, 0:1, :] for i in range(4))
    for s in range(1, segments):
        qr, qi, tr, ti = (ends[i, s : s + 1, :] for i in range(4))
        pr, pi = qr * pr - qi * pi, qr * pi + qi * pr
        sr, si = link((sr, si), (qr, qi, tr, ti))
    for i, v in enumerate((pr, pi, sr, si)):
        carries[sp, i : i + 1, :] = v

    def carry_copy(i, sending):
        there = (sp + i) % n
        slot = sp if sending else (sp + n - i) % n
        return pltpu.make_async_remote_copy(
            src_ref=carries.at[slot],
            dst_ref=carries.at[slot],
            send_sem=carry_send.at[i - 1],
            recv_sem=carry_recv.at[i - 1],
            device_id=(there, tp),
            device_id_type=MESH,
        )

    for i in range(1, n):
        carry_copy(i, True).start()
    for i in range(1, n):
        carry_copy(i, False).wait_recv()
    cr = jnp.zeros_like(pr)
    ci = jnp.zeros_like(pr)
    for d in range(n - 1):
        nr, ni = link((cr, ci), tuple(carries[d, i : i + 1, :] for i in range(4)))
        cr = jnp.where(d < sp, nr, cr)
        ci = jnp.where(d < sp, ni, ci)
    for s in range(segments):
        entry[0, s : s + 1, :] = cr
        entry[1, s : s + 1, :] = ci
        cr, ci = link((cr, ci), tuple(ends[i, s : s + 1, :] for i in range(4)))
    serve()

    for c in range(chunks):
        cols = pl.ds(c * lanes, lanes)

        def again(j, state):
            rows = pl.ds(pl.multiple_of(j * segments, segments), segments)
            dr, di = dre[rows, cols], dim[rows, cols]
            xr, xi = link(state, (dr, di, fre[rows, cols], fim[rows, cols]))
            proj[rows, 0:lanes] = xr
            proj[rows, lanes : 2 * lanes] = xi
            return xr, xi

        lax.fori_loop(0, length, again, (entry[0, :, cols], entry[1, :, cols]), unroll=4)
        ins = slice(c * kin, (c + 1) * kin)
        mech = jnp.dot(proj[...].astype(bf16), w_out_ref[c], preferred_element_type=f32)
        mech = mech + skip_ref[0:1, ins] * mixer_perm[:, ins].astype(f32)
        mixed_perm[:, ins] = jax.nn.gelu(mech).astype(bf16)
        if c % 2 == 1:
            serve()
    chan[tp] = jnp.dot(unperm_ref[...], mixed_perm[...], preferred_element_type=f32).astype(bf16)

    def tp_copy(buf, sems, i, sending):
        slot = tp if sending else (tp + ntp - i) % ntp
        return pltpu.make_async_remote_copy(
            src_ref=buf.at[slot],
            dst_ref=buf.at[slot],
            send_sem=sems[0].at[i - 1],
            recv_sem=sems[1].at[i - 1],
            device_id=(sp, (tp + i) % ntp),
            device_id_type=MESH,
        )

    chan_sems, upd_sems = (chan_send, chan_recv), (upd_send, upd_recv)
    for i in range(1, ntp):
        tp_copy(chan, chan_sems, i, True).start()
    serve()
    for i in range(1, ntp):
        tp_copy(chan, chan_sems, i, False).wait_recv()

    tile = 256

    @pl.loop(0, width // tile)
    def _(t):
        cols = pl.ds(pl.multiple_of(t * tile, tile), tile)
        v = jnp.zeros((tokens, tile), f32)
        g = jnp.zeros((tokens, tile), f32)
        for q in range(ntp):
            rows = slice(q * width, (q + 1) * width)
            v += jnp.dot(chan[q], value_ref[rows, cols], preferred_element_type=f32)
            g += jnp.dot(chan[q], gate_ref[rows, cols], preferred_element_type=f32)
        upd[tp, :, cols] = (resid_ref[:, cols].astype(f32) + v * jax.nn.sigmoid(g)).astype(bf16)

    for i in range(1, ntp):
        tp_copy(upd, upd_sems, i, True).start()
    serve()
    for i in range(1, ntp):
        tp_copy(upd, upd_sems, i, False).wait_recv()

    total = jnp.zeros((tokens, 1), f32)
    for q in range(ntp):
        u = upd[q].astype(f32)
        total += jnp.sum(u * u, axis=1, keepdims=True)
    inv = lax.rsqrt(total * (1.0 / (width * ntp)) + rms_eps)
    for q in range(ntp):
        cols = slice(q * width, (q + 1) * width)
        normed[:, cols] = (upd[q].astype(f32) * inv * gain_ref[0:1, cols]).astype(bf16)

    while queue and queue[0] < n - 1:
        serve()
    for c in own:
        c.wait()
    if queue and queue[0] == n - 1:
        serve()
    finish(0)

    @pl.loop(0, hidden.shape[1] // tile)
    def _(t):
        cols = pl.ds(pl.multiple_of(t * tile, tile), tile)
        r = jnp.dot(normed[...], whole[0, :, cols], preferred_element_type=f32)
        r = jnp.maximum(r, 0.0)
        hidden[:, cols] = (r * r).astype(bf16)

    while queue:
        serve()
    finish(1)

    per = width // tile

    def part_copy(i, sending):
        there = (tp + i) % ntp
        slot = tp if sending else (tp + ntp - i) % ntp
        return pltpu.make_async_remote_copy(
            src_ref=parts.at[i],
            dst_ref=landed.at[slot],
            send_sem=part_send.at[i - 1],
            recv_sem=part_recv.at[i - 1],
            device_id=(sp, there),
            device_id_type=MESH,
        )

    for i in (2, 1, 3, 0)[:ntp] if ntp == 4 else range(ntp - 1, -1, -1):
        there = (tp + i) % ntp

        @pl.loop(0, per)
        def _(t):
            rows = pl.ds(pl.multiple_of(there * width + t * tile, tile), tile)
            p = lax.dot_general(
                hidden[...],
                whole[1, rows, :],
                (((1,), (1,)), ((), ())),
                preferred_element_type=f32,
            )
            parts[i, t] = p.astype(bf16)

        if i > 0:
            part_copy(i, True).start()

    for i in range(1, ntp):
        part_copy(i, False).wait_recv()
    for t in range(per):
        cols = slice(t * tile, (t + 1) * tile)
        acc = parts[0, t].astype(f32)
        for i in range(1, ntp):
            acc += landed[(tp + i) % ntp, t].astype(f32)
        out_ref[:, cols] = (upd[tp, :, cols].astype(f32) + acc).astype(bf16)

    for which in range(2):
        for k in range(n - 1):
            for way in range(2):
                for part in range(pieces):
                    ring_copy(which, way, k, part, True).wait_send()
    for i in range(1, n):
        carry_copy(i, True).wait_send()
    for i in range(1, ntp):
        tp_copy(chan, chan_sems, i, True).wait_send()
        tp_copy(upd, upd_sems, i, True).wait_send()
        part_copy(i, True).wait_send()


def per_device(
    n,
    ntp,
    resid,
    mixer_in,
    log_step,
    decay_real,
    frequency,
    input_matrix,
    output_matrix,
    skip_gain,
    value_weight,
    gate_weight,
    norm_gain,
    up_weight,
    down_weight,
):
    tokens, width = mixer_in.shape
    groups, states = decay_real.shape
    per = width // groups
    bunch = min(128 // per, groups)
    chunks = groups // bunch
    kin, lanes = bunch * per, bunch * states
    features, units = value_weight.shape[0], up_weight.shape[1]
    length = tokens // segments
    modulus = decay_real * decay_real + frequency * frequency
    rates = jnp.stack(
        [decay_real, frequency, decay_real / modulus, frequency / modulus]
    ).reshape(4, groups * states)
    same = jnp.eye(bunch, dtype=bf16)
    w_in = input_matrix.astype(bf16).reshape(2, chunks, bunch, states, per)
    w_in = w_in.transpose(1, 2, 4, 0, 3)[:, :, :, :, None, :]
    w_in = (w_in * same[None, :, None, None, :, None]).reshape(chunks, kin, 2 * lanes)
    w_out = jnp.stack([output_matrix[0], -output_matrix[1]]).astype(bf16)
    w_out = w_out.reshape(2, chunks, bunch, per, states).transpose(1, 0, 2, 4, 3)
    w_out = (w_out[:, :, :, :, None, :] * same[None, None, :, None, :, None]).reshape(
        chunks, 2 * lanes, kin
    )
    step_perm = log_step.reshape(segments, length, groups).transpose(1, 0, 2)
    step_perm = step_perm.reshape(tokens, groups)
    row = jnp.arange(tokens)
    perm = (row[None, :] == ((row % segments) * length + row // segments)[:, None]).astype(bf16)
    pieces = 2
    total = groups * states
    tile = 256
    dma = pltpu.SemaphoreType.DMA
    vmem = pl.BlockSpec(memory_space=pltpu.VMEM)
    return pl.pallas_call(
        functools.partial(kernel, n, ntp),
        out_shape=jax.ShapeDtypeStruct((tokens, width), bf16),
        in_specs=[vmem] * 14,
        out_specs=vmem,
        scratch_shapes=[
            pltpu.VMEM((2, features, units), bf16),
            pltpu.VMEM((tokens, total), f32),
            pltpu.VMEM((tokens, total), f32),
            pltpu.VMEM((tokens, total), f32),
            pltpu.VMEM((tokens, total), f32),
            pltpu.VMEM((tokens, lanes), f32),
            pltpu.VMEM((tokens, 2 * lanes), f32),
            pltpu.VMEM((4, segments, total), f32),
            pltpu.VMEM((n, 4, total), f32),
            pltpu.VMEM((2, segments, total), f32),
            pltpu.VMEM((tokens, width), bf16),
            pltpu.VMEM((tokens, width), bf16),
            pltpu.VMEM((ntp, tokens, width), bf16),
            pltpu.VMEM((ntp, tokens, width), bf16),
            pltpu.VMEM((tokens, features), bf16),
            pltpu.VMEM((tokens, units), bf16),
            pltpu.VMEM((ntp, width // tile, tokens, tile), bf16),
            pltpu.VMEM((ntp, width // tile, tokens, tile), bf16),
            dma((2, 2, n - 1, pieces)),
            dma((2, 2, n - 1, pieces)),
            dma((2,)),
            dma((n - 1,)),
            dma((n - 1,)),
            dma((ntp - 1,)),
            dma((ntp - 1,)),
            dma((ntp - 1,)),
            dma((ntp - 1,)),
            dma((ntp - 1,)),
            dma((ntp - 1,)),
        ],
        compiler_params=pltpu.CompilerParams(
            collective_id=0, has_side_effects=True, vmem_limit_bytes=64 * 1024 * 1024 - 65536
        ),
    )(
        resid,
        mixer_in,
        step_perm,
        rates,
        w_in,
        w_out,
        skip_gain.reshape(1, width),
        value_weight,
        gate_weight,
        norm_gain.reshape(1, features),
        up_weight,
        down_weight,
        perm,
        perm.T,
    )


def solution(mesh):
    in_specs = (
        P("sp", "tp"),
        P("sp", "tp"),
        P("sp", "tp"),
        P("tp", None),
        P("tp", None),
        P(None, "tp", None, None),
        P(None, "tp", None, None),
        P("tp"),
        P(None, "tp"),
        P(None, "tp"),
        P(),
        P("sp", "tp"),
        P("sp", "tp"),
    )
    body = functools.partial(per_device, mesh.shape["sp"], mesh.shape["tp"])
    return jax.shard_map(
        body, mesh=mesh, in_specs=in_specs, out_specs=P("sp", "tp"), check_vma=False
    )
```

```python
import functools

import jax
import jax.numpy as jnp
import numpy as np
from jax import lax
from jax.experimental import pallas as pl
from jax.experimental.pallas import tpu as pltpu
from jax.sharding import PartitionSpec as P

rms_eps = 1e-06
segments = 8
MESH = pl.DeviceIdType.MESH
f32, bf16 = jnp.float32, jnp.bfloat16


def sine_cosine(x):
    y = x * x
    s = 1.0 + y * (-1 / 6 + y * (1 / 120 + y * (-1 / 5040 + y * (1 / 362880 + y * (-1 / 39916800)))))
    c = 1.0 + y * (
        -0.5
        + y * (1 / 24 + y * (-1 / 720 + y * (1 / 40320 + y * (-1 / 3628800 + y * (1 / 479001600)))))
    )
    return x * s, c


def expm1_small(y):
    return y * (
        1.0
        + y * (1 / 2 + y * (1 / 6 + y * (1 / 24 + y * (1 / 120 + y * (1 / 720 + y * (1 / 5040))))))
    )


def kernel(
    n,
    ntp,
    resid_ref,
    mixer_ref,
    step_ref,
    decay_ref,
    angle_ref,
    w_in_ref,
    w_out_ref,
    skip_ref,
    value_ref,
    gate_ref,
    gain_ref,
    up_ref,
    down_ref,
    perm_ref,
    unperm_ref,
    out_ref,
    whole,
    dre,
    dim,
    fre,
    fim,
    step_wide,
    proj,
    ends,
    carries,
    entry,
    mixer_perm,
    mixed_perm,
    chan,
    upd,
    normed,
    hidden,
    parts,
    landed,
    ring_send,
    ring_recv,
    own_sem,
    carry_send,
    carry_recv,
    chan_send,
    chan_recv,
    upd_send,
    upd_recv,
    part_send,
    part_recv,
):
    sp = lax.axis_index("sp")
    tp = lax.axis_index("tp")
    tokens, width = mixer_ref.shape
    block = up_ref.shape[0]
    pieces = ring_send.shape[3]
    piece = block // (2 * pieces)
    groups, states = decay_ref.shape
    each = width // groups
    bunch = min(128 // each, groups)
    chunks = groups // bunch
    lanes, kin = bunch * states, bunch * each
    length = tokens // segments

    odd = sp % 2
    pos = (1 - odd) * (sp // 2) + odd * (n - 1 - sp // 2)

    def at_pos(p):
        p = (p + 2 * n) % n
        high = p // (n // 2)
        return (1 - high) * 2 * p + high * (2 * (n - 1 - p) + 1)

    ahead, behind = at_pos(pos + 1), at_pos(pos - 1)

    barrier = pltpu.get_barrier_semaphore()
    for i in range(1, n):
        pl.semaphore_signal(barrier, inc=1, device_id=((sp + i) % n, tp), device_id_type=MESH)
    for i in range(1, ntp):
        pl.semaphore_signal(barrier, inc=1, device_id=(sp, (tp + i) % ntp), device_id_type=MESH)
    pl.semaphore_wait(barrier, n - 1 + ntp - 1)

    def rows_of(owner, way, part):
        return pl.ds(pl.multiple_of(owner * block + (way * pieces + part) * piece, piece), piece)

    def ring_copy(which, way, k, part, sending):
        source = (up_ref, down_ref)[which]
        sign = -1 if way == 0 else 1
        to = ahead if way == 0 else behind
        shift = k if sending else k + 1
        owner = at_pos(pos + sign * shift)
        slot = whole.at[which, rows_of(owner, way, part)]
        if k == 0 and sending:
            src = source.at[pl.ds((way * pieces + part) * piece, piece)]
        else:
            src = slot
        return pltpu.make_async_remote_copy(
            src_ref=src,
            dst_ref=slot,
            send_sem=ring_send.at[which, way, k, part],
            recv_sem=ring_recv.at[which, way, k, part],
            device_id=(to, tp),
            device_id_type=MESH,
        )

    def service(index):
        which, k = index // (n - 1), index % (n - 1)
        for part in range(pieces):
            for way in range(2):
                if k > 0:
                    ring_copy(which, way, k - 1, part, False).wait_recv()
                ring_copy(which, way, k, part, True).start()

    def finish(which):
        for part in range(pieces):
            for way in range(2):
                ring_copy(which, way, n - 2, part, False).wait_recv()

    queue = list(range(2 * (n - 1)))

    def serve(count=1):
        for _ in range(count):
            if queue:
                service(queue.pop(0))

    own = []
    for which, source in enumerate((up_ref, down_ref)):
        start = pl.multiple_of(sp * block, block)
        c = pltpu.make_async_copy(source, whole.at[which, pl.ds(start, block)], own_sem.at[which])
        c.start()
        own.append(c)
    serve()

    mixer_perm[...] = jnp.dot(
        perm_ref[...], mixer_ref[...], preferred_element_type=f32
    ).astype(bf16)
    highest = lax.Precision.HIGHEST
    step_size = jnp.dot(
        perm_ref[...].astype(f32),
        jnp.exp(step_ref[...]),
        precision=highest,
        preferred_element_type=f32,
    )

    def iota(shape, axis):
        return lax.broadcasted_iota(jnp.int32, shape, axis)

    def ones_where(mask, dtype=f32):
        return jnp.where(mask, 1.0, 0.0).astype(dtype)

    def belongs(rows, columns, span, first):
        gap = iota((rows, columns), 1) + first - iota((rows, columns), 0) * span
        return ones_where((gap >= 0) & (gap < span))

    def tiled(size, copies):
        shape = (size, size * copies)
        hits = jnp.zeros(shape, f32)
        for i in range(copies):
            hits += ones_where(iota(shape, 1) - iota(shape, 0) == i * size)
        return hits

    over_states = tiled(states, bunch)
    over_each = tiled(each, bunch).astype(bf16)
    agree = jnp.zeros((kin, lanes), f32)
    agree_t = jnp.zeros((lanes, kin), f32)
    for i in range(bunch):
        r, l = iota((kin, lanes), 0) - i * each, iota((kin, lanes), 1) - i * states
        agree += ones_where((r >= 0) & (r < each) & (l >= 0) & (l < states))
        r, l = iota((lanes, kin), 1) - i * each, iota((lanes, kin), 0) - i * states
        agree_t += ones_where((r >= 0) & (r < each) & (l >= 0) & (l < states))

    def wide_rate(table, c):
        spread = jnp.dot(table, over_states, precision=highest, preferred_element_type=f32)
        return jnp.sum(
            spread * belongs(groups, lanes, states, c * lanes), axis=0, keepdims=True
        )

    for c in range(chunks):
        cols = pl.ds(c * lanes, lanes)
        step_wide[...] = jnp.dot(
            step_size,
            belongs(groups, lanes, states, c * lanes),
            precision=highest,
            preferred_element_type=f32,
        )
        for i in range(2):
            matrix = jnp.dot(
                w_in_ref[i, c * lanes : (c + 1) * lanes, :].astype(bf16),
                over_each,
                preferred_element_type=f32,
            )
            proj[:, i * lanes : (i + 1) * lanes] = lax.dot_general(
                mixer_perm[:, c * kin : (c + 1) * kin],
                (matrix * agree_t).astype(bf16),
                (((1,), (1,)), ((), ())),
                preferred_element_type=f32,
            )
        rate_row = wide_rate(decay_ref[...], c)
        angle_row = wide_rate(angle_ref[...], c)
        modulus = rate_row * rate_row + angle_row * angle_row
        shape = (segments, lanes)
        rate = jnp.broadcast_to(rate_row, shape)
        half_angle = jnp.broadcast_to(angle_row * 0.5, shape)
        rate_n = jnp.broadcast_to(rate_row / modulus, shape)
        angle_n = jnp.broadcast_to(angle_row / modulus, shape)

        def one(j, state):
            pr, pi, sr, si = state
            rows = pl.ds(pl.multiple_of(j * segments, segments), segments)
            step = step_wide[rows, :]
            s, co = sine_cosine(half_angle * step)
            em = expm1_small(-rate * step)
            factor = 1.0 + em
            twice = 2.0 * s * s
            cos_r = 1.0 - twice
            dr = factor * cos_r
            di = factor * (2.0 * s * co)
            mr = em * cos_r - twice
            vr = di * angle_n - mr * rate_n
            vi = -di * rate_n - mr * angle_n
            a = proj[rows, 0:lanes]
            b = proj[rows, lanes : 2 * lanes]
            fr = vr * a - vi * b
            fi = vr * b + vi * a
            dre[rows, cols] = dr
            dim[rows, cols] = di
            fre[rows, cols] = fr
            fim[rows, cols] = fi
            return (
                dr * pr - di * pi,
                dr * pi + di * pr,
                dr * sr - di * si + fr,
                dr * si + di * sr + fi,
            )

        zero = jnp.zeros(shape, f32)
        last = lax.fori_loop(0, length, one, (zero + 1.0, zero, zero, zero), unroll=2)
        for i in range(4):
            ends[i, :, cols] = last[i]
        serve()

    def link(earlier, later):
        return (
            later[0] * earlier[0] - later[1] * earlier[1] + later[2],
            later[0] * earlier[1] + later[1] * earlier[0] + later[3],
        )

    pr, pi, sr, si = (ends[i, 0:1, :] for i in range(4))
    for s in range(1, segments):
        qr, qi, tr, ti = (ends[i, s : s + 1, :] for i in range(4))
        pr, pi = qr * pr - qi * pi, qr * pi + qi * pr
        sr, si = link((sr, si), (qr, qi, tr, ti))
    for i, v in enumerate((pr, pi, sr, si)):
        carries[sp, i : i + 1, :] = v

    def carry_copy(i, sending):
        there = (sp + i) % n
        slot = sp if sending else (sp + n - i) % n
        return pltpu.make_async_remote_copy(
            src_ref=carries.at[slot],
            dst_ref=carries.at[slot],
            send_sem=carry_send.at[i - 1],
            recv_sem=carry_recv.at[i - 1],
            device_id=(there, tp),
            device_id_type=MESH,
        )

    for i in range(1, n):
        carry_copy(i, True).start()
    for i in range(1, n):
        carry_copy(i, False).wait_recv()
    cr = jnp.zeros_like(pr)
    ci = jnp.zeros_like(pr)
    for d in range(n - 1):
        nr, ni = link((cr, ci), tuple(carries[d, i : i + 1, :] for i in range(4)))
        cr = jnp.where(d < sp, nr, cr)
        ci = jnp.where(d < sp, ni, ci)
    for s in range(segments):
        entry[0, s : s + 1, :] = cr
        entry[1, s : s + 1, :] = ci
        cr, ci = link((cr, ci), tuple(ends[i, s : s + 1, :] for i in range(4)))
    serve()

    for c in range(chunks):
        cols = pl.ds(c * lanes, lanes)

        def again(j, state):
            rows = pl.ds(pl.multiple_of(j * segments, segments), segments)
            dr, di = dre[rows, cols], dim[rows, cols]
            xr, xi = link(state, (dr, di, fre[rows, cols], fim[rows, cols]))
            proj[rows, 0:lanes] = xr
            proj[rows, lanes : 2 * lanes] = xi
            return xr, xi

        lax.fori_loop(0, length, again, (entry[0, :, cols], entry[1, :, cols]), unroll=4)
        ins = slice(c * kin, (c + 1) * kin)
        mech = jnp.zeros((tokens, kin), f32)
        for i in range(2):
            matrix = jnp.dot(
                w_out_ref[i, c * kin : (c + 1) * kin, :].astype(bf16),
                over_states.astype(bf16),
                preferred_element_type=f32,
            )
            mech += (1 - 2 * i) * lax.dot_general(
                proj[:, i * lanes : (i + 1) * lanes].astype(bf16),
                (matrix * agree).astype(bf16),
                (((1,), (1,)), ((), ())),
                preferred_element_type=f32,
            )
        mech = mech + skip_ref[0:1, ins] * mixer_perm[:, ins].astype(f32)
        mixed_perm[:, ins] = jax.nn.gelu(mech).astype(bf16)
        if c % 2 == 1:
            serve()
    chan[tp] = jnp.dot(unperm_ref[...], mixed_perm[...], preferred_element_type=f32).astype(bf16)

    def tp_copy(buf, sems, i, sending):
        slot = tp if sending else (tp + ntp - i) % ntp
        return pltpu.make_async_remote_copy(
            src_ref=buf.at[slot],
            dst_ref=buf.at[slot],
            send_sem=sems[0].at[i - 1],
            recv_sem=sems[1].at[i - 1],
            device_id=(sp, (tp + i) % ntp),
            device_id_type=MESH,
        )

    chan_sems, upd_sems = (chan_send, chan_recv), (upd_send, upd_recv)
    for i in range(1, ntp):
        tp_copy(chan, chan_sems, i, True).start()
    serve()
    for i in range(1, ntp):
        tp_copy(chan, chan_sems, i, False).wait_recv()

    tile = 256

    @pl.loop(0, width // tile)
    def _(t):
        cols = pl.ds(pl.multiple_of(t * tile, tile), tile)
        v = jnp.zeros((tokens, tile), f32)
        g = jnp.zeros((tokens, tile), f32)
        for q in range(ntp):
            rows = slice(q * width, (q + 1) * width)
            v += jnp.dot(chan[q], value_ref[rows, cols], preferred_element_type=f32)
            g += jnp.dot(chan[q], gate_ref[rows, cols], preferred_element_type=f32)
        upd[tp, :, cols] = (resid_ref[:, cols].astype(f32) + v * jax.nn.sigmoid(g)).astype(bf16)

    for i in range(1, ntp):
        tp_copy(upd, upd_sems, i, True).start()
    serve()
    for i in range(1, ntp):
        tp_copy(upd, upd_sems, i, False).wait_recv()

    total = jnp.zeros((tokens, 1), f32)
    for q in range(ntp):
        u = upd[q].astype(f32)
        total += jnp.sum(u * u, axis=1, keepdims=True)
    inv = lax.rsqrt(total * (1.0 / (width * ntp)) + rms_eps)
    for q in range(ntp):
        cols = slice(q * width, (q + 1) * width)
        normed[:, cols] = (upd[q].astype(f32) * inv * gain_ref[0:1, cols]).astype(bf16)

    while queue and queue[0] < n - 1:
        serve()
    for c in own:
        c.wait()
    if queue and queue[0] == n - 1:
        serve()
    finish(0)

    @pl.loop(0, hidden.shape[1] // tile)
    def _(t):
        cols = pl.ds(pl.multiple_of(t * tile, tile), tile)
        r = jnp.dot(normed[...], whole[0, :, cols], preferred_element_type=f32)
        r = jnp.maximum(r, 0.0)
        hidden[:, cols] = (r * r).astype(bf16)

    per = 2 * n // ntp
    half = block // 2

    def part_copy(h):
        return pltpu.make_async_remote_copy(
            src_ref=parts.at[h],
            dst_ref=landed.at[tp, h % per],
            send_sem=part_send.at[h],
            recv_sem=part_recv.at[tp, h % per],
            device_id=(sp, h // per),
            device_id_type=MESH,
        )

    def down_part(owner, way):
        h = 2 * owner + way
        rows = pl.ds(pl.multiple_of(h * half, half), half)
        p = lax.dot_general(
            hidden[...],
            whole[1, rows, :],
            (((1,), (1,)), ((), ())),
            preferred_element_type=f32,
        )
        parts[h] = p.astype(bf16)

        @pl.when(h // per != tp)
        def _():
            part_copy(h).start()

    down_part(sp, 0)
    down_part(sp, 1)
    for k in range(n - 1):
        if k < n - 2:
            while queue and queue[0] <= n + k:
                serve()
        else:
            finish(1)
        down_part(at_pos(pos - k - 1), 0)
        down_part(at_pos(pos + k + 1), 1)

    for i in range(1, ntp):
        there = (tp + i) % ntp
        for t in range(per):
            pltpu.make_async_remote_copy(
                src_ref=parts.at[t],
                dst_ref=landed.at[there, t],
                send_sem=part_send.at[t],
                recv_sem=part_recv.at[there, t],
                device_id=(sp, there),
                device_id_type=MESH,
            ).wait_recv()
    for t in range(per):
        cols = slice(t * half, (t + 1) * half)
        acc = parts[tp * per + t].astype(f32)
        for i in range(1, ntp):
            acc += landed[(tp + i) % ntp, t].astype(f32)
        out_ref[:, cols] = (upd[tp, :, cols].astype(f32) + acc).astype(bf16)

    for which in range(2):
        for k in range(n - 1):
            for way in range(2):
                for part in range(pieces):
                    ring_copy(which, way, k, part, True).wait_send()
    for i in range(1, n):
        carry_copy(i, True).wait_send()
    for i in range(1, ntp):
        tp_copy(chan, chan_sems, i, True).wait_send()
        tp_copy(upd, upd_sems, i, True).wait_send()
    for h in range(2 * n):

        @pl.when(h // per != tp)
        def _():
            part_copy(h).wait_send()


def per_device(
    n,
    ntp,
    resid,
    mixer_in,
    log_step,
    decay_real,
    frequency,
    input_matrix,
    output_matrix,
    skip_gain,
    value_weight,
    gate_weight,
    norm_gain,
    up_weight,
    down_weight,
):
    tokens, width = mixer_in.shape
    groups, states = decay_real.shape
    per = width // groups
    bunch = min(128 // per, groups)
    chunks = groups // bunch
    kin, lanes = bunch * per, bunch * states
    features, units = value_weight.shape[0], up_weight.shape[1]
    length = tokens // segments
    row = np.arange(tokens)
    perm = (row[None, :] == ((row % segments) * length + row // segments)[:, None]).astype(np.float32)
    pieces = 2
    total = groups * states
    dma = pltpu.SemaphoreType.DMA
    vmem = pl.BlockSpec(memory_space=pltpu.VMEM)
    return pl.pallas_call(
        functools.partial(kernel, n, ntp),
        out_shape=jax.ShapeDtypeStruct((tokens, width), bf16),
        in_specs=[vmem] * 15,
        out_specs=vmem,
        scratch_shapes=[
            pltpu.VMEM((2, features, units), bf16),
            pltpu.VMEM((tokens, total), f32),
            pltpu.VMEM((tokens, total), f32),
            pltpu.VMEM((tokens, total), f32),
            pltpu.VMEM((tokens, total), f32),
            pltpu.VMEM((tokens, lanes), f32),
            pltpu.VMEM((tokens, 2 * lanes), f32),
            pltpu.VMEM((4, segments, total), f32),
            pltpu.VMEM((n, 4, total), f32),
            pltpu.VMEM((2, segments, total), f32),
            pltpu.VMEM((tokens, width), bf16),
            pltpu.VMEM((tokens, width), bf16),
            pltpu.VMEM((ntp, tokens, width), bf16),
            pltpu.VMEM((ntp, tokens, width), bf16),
            pltpu.VMEM((tokens, features), bf16),
            pltpu.VMEM((tokens, units), bf16),
            pltpu.VMEM((2 * n, tokens, features // (2 * n)), bf16),
            pltpu.VMEM((ntp, 2 * n // ntp, tokens, features // (2 * n)), bf16),
            dma((2, 2, n - 1, pieces)),
            dma((2, 2, n - 1, pieces)),
            dma((2,)),
            dma((n - 1,)),
            dma((n - 1,)),
            dma((ntp - 1,)),
            dma((ntp - 1,)),
            dma((ntp - 1,)),
            dma((ntp - 1,)),
            dma((2 * n,)),
            dma((ntp, 2 * n // ntp)),
        ],
        compiler_params=pltpu.CompilerParams(
            collective_id=0, has_side_effects=True, vmem_limit_bytes=64 * 1024 * 1024 - 65536
        ),
    )(
        resid,
        mixer_in,
        log_step,
        decay_real,
        frequency,
        input_matrix.reshape(2, groups * states, per),
        output_matrix.reshape(2, groups * per, states),
        skip_gain.reshape(1, width),
        value_weight,
        gate_weight,
        norm_gain.reshape(1, features),
        up_weight,
        down_weight,
        jnp.asarray(perm, bf16),
        jnp.asarray(perm.T, bf16),
    )


def solution(mesh):
    in_specs = (
        P("sp", "tp"),
        P("sp", "tp"),
        P("sp", "tp"),
        P("tp", None),
        P("tp", None),
        P(None, "tp", None, None),
        P(None, "tp", None, None),
        P("tp"),
        P(None, "tp"),
        P(None, "tp"),
        P(),
        P("sp", "tp"),
        P("sp", "tp"),
    )
    body = functools.partial(per_device, mesh.shape["sp"], mesh.shape["tp"])
    return jax.shard_map(
        body, mesh=mesh, in_specs=in_specs, out_specs=P("sp", "tp"), check_vma=False
    )
```
